32 devices in a mesh: sp: 4 (over z), fs: 4 (over y, x), tp: 2 (over core).
Axes of the slice: x: 2, y: 2, z: 4, core: 2. Of those that a mesh axis runs over, the one named last changes fastest.
Arguments:
- tokens: bfloat16 [2, 512, 1024], P('tp', 'sp'), may hold values from -6 to 6
- in_gain: float32 [1024], replicated, may hold values from 0.1 to 1.9
- query_weight: bfloat16 [1024, 1024], P('sp', 'fs'), may hold values from -0.1875 to 0.1875
- key_weight: bfloat16 [1024, 256], P('sp', 'fs'), may hold values from -0.1875 to 0.1875
- value_weight: bfloat16 [1024, 256], P('sp', 'fs'), may hold values from -0.1875 to 0.1875
- attn_gate_weight: bfloat16 [1024, 1024], P('sp', 'fs'), may hold values from -0.1875 to 0.1875
- state_in_weight: bfloat16 [1024, 512], P('sp', 'fs'), may hold values from -0.1875 to 0.1875
- state_gate_weight: bfloat16 [1024, 512], P('sp', 'fs'), may hold values from -0.1875 to 0.1875
- sink_logits: float32 [16], P('fs'), may hold values from 2 to 6
- decay_rate: float32 [32, 64], P('fs'), may hold values from 0.05 to 1.5
- rotation: float32 [32, 64], P('fs'), may hold values from 0.3 to 1.5
- step_size: float32 [32], P('fs'), may hold values from 0.5 to 2
- input_real: float32 [32, 64, 16], P('fs'), may hold values from -1 to 1
- input_imag: float32 [32, 64, 16], P('fs'), may hold values from -1 to 1
- output_real: float32 [32, 16, 64], P('fs'), may hold values from -0.0234375 to 0.0234375
- output_imag: float32 [32, 16, 64], P('fs'), may hold values from -0.0234375 to 0.0234375
- skip_scale: float32 [512], P('fs'), may hold values from -4 to 4
- focus_result_coefficients: bfloat16 [1024, 1024], P('fs', 'sp'), may hold values from -1 to 1
- state_out_weight: bfloat16 [512, 1024], P('fs', 'sp'), may hold values from -0.25 to 0.25
- out_gain: float32 [1024], P('fs'), may hold values from 0.1 to 1.9
Outputs:
- layer_output: bfloat16 [2, 512, 1024], P('tp', 'sp', 'fs')
The draws below stay inside these ranges and needn't reach their ends.
All inputs are finite; a program needn't handle non-finite values.
Results may differ from the reference program's by a relative error of at most 0.015.
Values may be sent and summed in bfloat16 or wider, within the bound.
A program may use at most 64 MiB of HBM per device.

```python
import math
import jax
import jax.numpy as jnp
from jax import lax

D = 1024
HEAD_DIM = 64
Q_HEADS = 16
KV_HEADS = 4
WINDOW = 128
GROUP = 16
GROUPS = 32
STATE = 64
TOK_DEV = 128
SEQ = 512
BATCH = 2
Q_WIDTH = 1024
KV_WIDTH = 256
SSM_WIDTH = 512


def level_of(key, extent, cuts, least, top_value):
    factor_of = 1.0
    for axis_at, shards_of in cuts:
        steps = jax.random.uniform(jax.random.fold_in(jax.random.fold_in(key, 6), axis_at), (shards_of,), jnp.float32, least / len(cuts), top_value / len(cuts))
        factor_of = factor_of * jnp.repeat(jnp.exp(steps), extent[axis_at] // shards_of).reshape((-1,) + (1,) * (len(extent) - 1 - axis_at))
    return factor_of


def gaussian(rng, dims, width, reach, split=(), kind=jnp.bfloat16):
    array = width * jax.random.normal(rng, dims, jnp.float32)
    if split:
        array = array * level_of(rng, dims, split, -0.22, 0.18)
    return jnp.clip(array, -reach, reach).astype(kind)


def setup_inputs(seed: int = 0) -> dict:
    key_list = jax.random.split(jax.random.key(seed), 21)
    return {
        "tokens": gaussian(key_list[0], (BATCH, SEQ, D), 1.0, 6.0, ((0, 2), (1, 4))),
        "in_gain": jnp.clip(1.0 + 0.18 * jax.random.normal(key_list[1], (D,), jnp.float32), 0.1, 1.9),
        "query_weight": gaussian(key_list[2], (D, Q_WIDTH), D ** -0.5, 0.1875, ((0, 4), (1, 4))),
        "key_weight": gaussian(key_list[3], (D, KV_WIDTH), D ** -0.5, 0.1875, ((0, 4), (1, 4))),
        "value_weight": gaussian(key_list[4], (D, KV_WIDTH), D ** -0.5, 0.1875, ((0, 4), (1, 4))),
        "attn_gate_weight": gaussian(key_list[5], (D, Q_WIDTH), D ** -0.5, 0.1875, ((0, 4), (1, 4))),
        "state_in_weight": gaussian(key_list[6], (D, SSM_WIDTH), D ** -0.5, 0.1875, ((0, 4), (1, 4))),
        "state_gate_weight": gaussian(key_list[7], (D, SSM_WIDTH), D ** -0.5, 0.1875, ((0, 4), (1, 4))),
        "sink_logits": jnp.clip(2.0 + 4.0 * jax.random.uniform(key_list[8], (Q_HEADS,), jnp.float32) ** level_of(key_list[8], (Q_HEADS,), ((0, 4),), -0.2, 0.2), 2.0, 6.0),
        "decay_rate": jnp.clip(jnp.exp(math.log(1.5) - 3.4011974 * jax.random.uniform(key_list[9], (GROUPS, STATE), jnp.float32) ** level_of(key_list[9], (GROUPS, STATE), ((0, 4),), -0.2, 0.2)), 0.05, 1.5),
        "rotation": jnp.clip(0.3 + 1.2 * jax.random.uniform(key_list[10], (GROUPS, STATE), jnp.float32) ** level_of(key_list[10], (GROUPS, STATE), ((0, 4),), -0.2, 0.2), 0.3, 1.5),
        "step_size": jnp.clip(jnp.exp(math.log(2.0) - 1.3862944 * jax.random.uniform(key_list[11], (GROUPS,), jnp.float32) ** level_of(key_list[11], (GROUPS,), ((0, 4),), -0.2, 0.2)), 0.5, 2.0),
        "input_real": gaussian(key_list[12], (GROUPS, STATE, GROUP), (2 * GROUP) ** -0.5, 1.0, ((0, 4),), jnp.float32),
        "input_imag": gaussian(key_list[13], (GROUPS, STATE, GROUP), (2 * GROUP) ** -0.5, 1.0, ((0, 4),), jnp.float32),
        "output_real": gaussian(key_list[14], (GROUPS, GROUP, STATE), (2 * STATE * SEQ) ** -0.5, 0.0234375, ((0, 4),), jnp.float32),
        "output_imag": gaussian(key_list[15], (GROUPS, GROUP, STATE), (2 * STATE * SEQ) ** -0.5, 0.0234375, ((0, 4),), jnp.float32),
        "skip_scale": gaussian(key_list[16], (SSM_WIDTH,), 1.0, 4.0, ((0, 4),), jnp.float32),
        "focus_result_coefficients": gaussian(key_list[17], (Q_WIDTH, D), (Q_WIDTH // 32) ** -0.5, 1.0, ((0, 4), (1, 4))),
        "state_out_weight": gaussian(key_list[18], (SSM_WIDTH, D), SSM_WIDTH ** -0.5, 0.25, ((0, 4), (1, 4))),
        "out_gain": jnp.clip(1.0 + 0.18 * jax.random.normal(key_list[19], (D,), jnp.float32), 0.1, 1.9),
    }


epsilon = 1e-05
theta_base = 10000.0

def layer_norm(values, gain):
    center = lax.optimization_barrier(jnp.mean(values, axis=-1, keepdims=True))
    spread = lax.optimization_barrier(jnp.mean(jnp.square(values - center), axis=-1, keepdims=True))
    return (values - center) * lax.rsqrt(spread + epsilon) * gain

def rotate(values, positions):
    half = HEAD_DIM // 2
    inv_freq = jnp.power(theta_base, -jnp.arange(half, dtype=jnp.float32) / half)
    angles = positions.astype(jnp.float32)[:, None] * inv_freq
    cosine = jnp.cos(angles)[:, None, :]
    sine = jnp.sin(angles)[:, None, :]
    first = values[..., :half].astype(jnp.float32)
    second = values[..., half:].astype(jnp.float32)
    turned = jnp.concatenate([first * cosine - second * sine, second * cosine + first * sine], axis=-1)
    return turned.astype(jnp.bfloat16)

def discretize(decay_rate, rotation, step_size, input_real, input_imag, sequence_extent):
    real_rate = -decay_rate / sequence_extent
    time_step = step_size[:, None]
    magnitude = jnp.exp(real_rate * time_step)
    decay_real = magnitude * jnp.cos(rotation * time_step)
    decay_imag = magnitude * jnp.sin(rotation * time_step)
    denominator = real_rate * real_rate + rotation * rotation
    factor_real = ((decay_real - 1.0) * real_rate + decay_imag * rotation) / denominator
    factor_imag = (decay_imag * real_rate - (decay_real - 1.0) * rotation) / denominator
    drive_real = factor_real[..., None] * input_real - factor_imag[..., None] * input_imag
    drive_imag = factor_real[..., None] * input_imag + factor_imag[..., None] * input_real
    return (decay_real, decay_imag, drive_real, drive_imag)

def window_attention(queries, key_rows, value_rows, sink_logits):
    batch_count, sequence_extent = (queries.shape[0], queries.shape[1])
    per_group = Q_HEADS // KV_HEADS
    padded_keys = jnp.pad(key_rows, ((0, 0), (WINDOW, 0), (0, 0), (0, 0)))
    padded_values = jnp.pad(value_rows, ((0, 0), (WINDOW, 0), (0, 0), (0, 0)))
    block_count = sequence_extent // TOK_DEV
    sink = sink_logits.reshape(KV_HEADS, per_group)[None, :, :, None, None]

    def one_block(index):
        start = index * TOK_DEV
        grouped = lax.dynamic_slice_in_dim(queries, start, TOK_DEV, 1).astype(jnp.float32)
        grouped = grouped.reshape(batch_count, TOK_DEV, KV_HEADS, per_group, HEAD_DIM)
        near_keys = lax.dynamic_slice_in_dim(padded_keys, start, TOK_DEV + WINDOW, 1).astype(jnp.float32)
        near_values = lax.dynamic_slice_in_dim(padded_values, start, TOK_DEV + WINDOW, 1).astype(jnp.float32)
        scores = jnp.einsum('bqkrd,bckd->bkrqc', grouped, near_keys) * HEAD_DIM ** (-0.5)
        query_pos = start + jnp.arange(TOK_DEV, dtype=jnp.int32)
        key_pos = start - WINDOW + jnp.arange(TOK_DEV + WINDOW, dtype=jnp.int32)
        differ = query_pos[:, None] - key_pos[None, :]
        allowed = (differ >= 0) & (differ < WINDOW) & (key_pos >= 0)[None, :]
        scores = jnp.where(allowed[None, None, None], scores, -jnp.inf)
        largest = jnp.maximum(lax.optimization_barrier(jnp.max(scores, axis=-1, keepdims=True)), sink)
        weights = jnp.exp(scores - largest)
        weights = weights / (lax.optimization_barrier(jnp.sum(weights, axis=-1, keepdims=True)) + jnp.exp(sink - largest))
        rounded = lax.optimization_barrier(weights.astype(jnp.bfloat16))
        attended = jnp.einsum('bkrqc,bckd->bqkrd', rounded.astype(jnp.float32), near_values)
        return attended.reshape(batch_count, TOK_DEV, Q_WIDTH)
    blocks = lax.map(one_block, jnp.arange(block_count, dtype=jnp.int32))
    return jnp.transpose(blocks, (1, 0, 2, 3)).reshape(batch_count, sequence_extent, Q_WIDTH)

def reference(tokens, in_gain, query_weight, key_weight, value_weight, attn_gate_weight, state_in_weight, state_gate_weight, sink_logits, decay_rate, rotation, step_size, input_real, input_imag, output_real, output_imag, skip_scale, focus_result_coefficients, state_out_weight, out_gain):
    batch_count, sequence_extent = (tokens.shape[0], tokens.shape[1])
    highest = lax.Precision.HIGHEST
    normed = layer_norm(tokens.astype(jnp.float32), in_gain).astype(jnp.bfloat16)
    flat_rows = normed.reshape(batch_count * sequence_extent, D)

    def project(number_grid):
        result = jnp.dot(flat_rows, number_grid, preferred_element_type=jnp.float32).astype(jnp.bfloat16)
        return result.reshape(batch_count, sequence_extent, number_grid.shape[1])
    positions = jnp.arange(sequence_extent, dtype=jnp.int32)
    queries = rotate(project(query_weight).reshape(batch_count, sequence_extent, Q_HEADS, HEAD_DIM), positions)
    key_rows = rotate(project(key_weight).reshape(batch_count, sequence_extent, KV_HEADS, HEAD_DIM), positions)
    value_rows = project(value_weight).reshape(batch_count, sequence_extent, KV_HEADS, HEAD_DIM)
    attn_gate = project(attn_gate_weight)
    state_input = project(state_in_weight)
    state_gate = project(state_gate_weight)
    attended = window_attention(queries, key_rows, value_rows, sink_logits)
    gated_attn = (jax.nn.sigmoid(attn_gate.astype(jnp.float32)) * attended).astype(jnp.bfloat16)
    decay_real, decay_imag, drive_real, drive_imag = discretize(decay_rate, rotation, step_size, input_real, input_imag, SEQ)
    inputs_float = state_input.astype(jnp.float32).reshape(batch_count, sequence_extent, GROUPS, GROUP)
    push_real = jnp.einsum('bsgh,gph->sbgp', inputs_float, drive_real, precision=highest)
    push_imag = jnp.einsum('bsgh,gph->sbgp', inputs_float, drive_imag, precision=highest)

    def advance(carry, pushes):
        state_real, state_imag = carry
        new_real = decay_real * state_real - decay_imag * state_imag + pushes[0]
        new_imag = decay_real * state_imag + decay_imag * state_real + pushes[1]
        return ((new_real, new_imag), (new_real, new_imag))
    nothing_values = jnp.zeros((batch_count, GROUPS, STATE), jnp.float32)
    _, (all_real, all_imag) = lax.scan(advance, (nothing_values, nothing_values), (push_real, push_imag))
    final_reading = jnp.einsum('sbgp,ghp->bsgh', all_real, output_real, precision=highest) - jnp.einsum('sbgp,ghp->bsgh', all_imag, output_imag, precision=highest)
    final_reading = final_reading + skip_scale.reshape(GROUPS, GROUP) * inputs_float
    final_reading = final_reading.reshape(batch_count, sequence_extent, SSM_WIDTH)
    gated_state = (jax.nn.gelu(final_reading, approximate=False) * jax.nn.sigmoid(state_gate.astype(jnp.float32))).astype(jnp.bfloat16)
    mixed = jnp.dot(gated_attn.reshape(-1, Q_WIDTH), focus_result_coefficients, preferred_element_type=jnp.float32) + jnp.dot(gated_state.reshape(-1, SSM_WIDTH), state_out_weight, preferred_element_type=jnp.float32)
    result = layer_norm(mixed, out_gain).astype(jnp.bfloat16)
    return result.reshape(batch_count, sequence_extent, D)
```

```python
import numpy as np
import jax
import jax.numpy as jnp
from jax import lax
from jax.sharding import PartitionSpec as P

HEAD_DIM = 64
WINDOW = 128
GROUP = 16

epsilon = 1e-05
theta_base = 10000.0


def shifted(value, axis, steps):
    count = lax.axis_size(axis)
    return lax.ppermute(value, axis, [(i, i + steps) for i in range(count - steps)])


def turned(value, axis, steps):
    count = lax.axis_size(axis)
    return lax.ppermute(value, axis, [(i, (i + steps) % count) for i in range(count)])


def dot(a, b):
    return jnp.dot(a, b, preferred_element_type=jnp.float32)


def dot_exact(a, b):
    return jnp.dot(a, b, preferred_element_type=jnp.float32, precision=lax.Precision.HIGHEST)


def times(a, b):
    return a[0] * b[0] - a[1] * b[1], a[0] * b[1] + a[1] * b[0]


def layer_norm(values, gain):
    center = jnp.mean(values, axis=-1, keepdims=True)
    spread = jnp.mean(jnp.square(values - center), axis=-1, keepdims=True)
    return (values - center) * lax.rsqrt(spread + epsilon) * gain


def turn_matrix(width):
    half = HEAD_DIM // 2
    matrix = np.zeros((width, width), np.float32)
    for column in range(width):
        if column % HEAD_DIM < half:
            matrix[column + half, column] = -1.0
        else:
            matrix[column - half, column] = 1.0
    return matrix


def powers(rate, angle, exponents):
    size = jnp.exp(exponents * rate)
    return size * jnp.cos(exponents * angle), size * jnp.sin(exponents * angle)


def spread_powers(rate, angle, count, sign):
    fine = 16 if count % 16 == 0 else count
    low = powers(rate, angle, sign * jnp.arange(fine, dtype=jnp.float32)[:, None])
    high = powers(rate, angle, sign * fine * jnp.arange(count // fine, dtype=jnp.float32)[:, None])
    product = times(tuple(h[:, None, :] for h in high), tuple(l[None] for l in low))
    return tuple(p.reshape(count, -1) for p in product)


def block_diagonal(blocks):
    groups, rows, columns = blocks.shape
    eye = jnp.eye(groups, dtype=blocks.dtype)
    return (blocks[:, :, None, :] * eye[:, None, :, None]).reshape(groups * rows, groups * columns)


def window_attention(queries, near_keys, near_values, sink_logits, offset, hop_count):
    extent = queries.shape[0]
    kv_local = near_keys.shape[1] // HEAD_DIM
    per_group = queries.shape[1] // HEAD_DIM // kv_local
    query_pos = offset + jnp.arange(extent, dtype=jnp.int32)
    key_pos = offset - hop_count * extent + jnp.arange((hop_count + 1) * extent, dtype=jnp.int32)
    differ = query_pos[:, None] - key_pos[None, :]
    allowed = (differ >= 0) & (differ < WINDOW) & (key_pos >= 0)[None, :]
    results = []
    for head in range(kv_local):
        keys = near_keys[:, head * HEAD_DIM:(head + 1) * HEAD_DIM]
        values = near_values[:, head * HEAD_DIM:(head + 1) * HEAD_DIM]
        start = head * per_group
        grouped = jnp.concatenate(
            [queries[:, (start + r) * HEAD_DIM:(start + r + 1) * HEAD_DIM] for r in range(per_group)], axis=0
        )
        scores = lax.dot_general(
            grouped, keys, (((1,), (1,)), ((), ())), preferred_element_type=jnp.float32
        ) * HEAD_DIM ** (-0.5)
        scores = scores.reshape(per_group, extent, -1)
        scores = jnp.where(allowed[None], scores, -jnp.inf)
        sink = sink_logits[start:start + per_group][:, None, None]
        largest = jnp.maximum(jnp.max(scores, axis=-1, keepdims=True), sink)
        weights = jnp.exp(scores - largest)
        weights = weights / (jnp.sum(weights, axis=-1, keepdims=True) + jnp.exp(sink - largest))
        weights = weights.astype(jnp.bfloat16).reshape(per_group * extent, -1)
        attended = dot(weights, values)
        results += [attended[r * extent:(r + 1) * extent] for r in range(per_group)]
    return jnp.concatenate(results, axis=1)


def on_device(
    tokens,
    in_gain,
    query_weight,
    key_weight,
    value_weight,
    attn_gate_weight,
    state_in_weight,
    state_gate_weight,
    sink_logits,
    decay_rate,
    rotation,
    step_size,
    input_real,
    input_imag,
    output_real,
    output_imag,
    skip_scale,
    focus_result_coefficients,
    state_out_weight,
    out_gain,
):
    extent, width = tokens.shape[1], tokens.shape[2]
    count = lax.axis_size("sp")
    mine = lax.axis_index("sp")
    offset = mine * extent
    total_length = extent * count
    own_in = jnp.concatenate(
        [query_weight, key_weight, value_weight, attn_gate_weight, state_in_weight, state_gate_weight], axis=1
    )
    own_out = jnp.concatenate([focus_result_coefficients, state_out_weight], axis=0)
    in_pieces = [own_in] + [turned(own_in, "sp", d) for d in range(1, count)]
    out_pieces = [own_out] + [turned(own_out, "sp", d) for d in range(1, count)]

    step = jnp.repeat(step_size, decay_rate.shape[1])[None, :]
    states = decay_rate.shape[0] * decay_rate.shape[1]
    real_rate = -decay_rate.reshape(1, states) / total_length
    imag_rate = rotation.reshape(1, states)
    rate, angle = real_rate * step, imag_rate * step
    one = jnp.ones((1, 1), jnp.float32)
    abar = powers(rate, angle, one)
    denominator = real_rate * real_rate + imag_rate * imag_rate
    factor = (
        ((abar[0] - 1.0) * real_rate + abar[1] * imag_rate) / denominator,
        (abar[1] * real_rate - (abar[0] - 1.0) * imag_rate) / denominator,
    )
    forward = spread_powers(rate, angle, extent, 1.0)
    inverse = times(factor, spread_powers(rate, angle, extent, -1.0))
    whole_block = powers(rate, angle, extent * one)
    drive_in = jnp.concatenate(
        [block_diagonal(jnp.swapaxes(m, 1, 2)) for m in (input_real, input_imag)], axis=1
    )
    read_out = jnp.concatenate(
        [block_diagonal(jnp.swapaxes(m, 1, 2)) for m in (output_real, -output_imag)], axis=0
    )

    normed = layer_norm(tokens[0].astype(jnp.float32), in_gain).astype(jnp.bfloat16)
    depth = own_in.shape[0]
    totals = None
    for d, piece in enumerate(in_pieces):
        owner = lax.rem(mine - d + count, count)
        part = dot(lax.dynamic_slice_in_dim(normed, owner * depth, depth, 1), piece)
        totals = part if totals is None else totals + part
    projected = totals.astype(jnp.bfloat16)
    q_wide, kv_wide, ssm_wide = query_weight.shape[1], key_weight.shape[1], state_in_weight.shape[1]
    cuts = [q_wide, q_wide + kv_wide, q_wide + 2 * kv_wide, 2 * q_wide + 2 * kv_wide,
            2 * q_wide + 2 * kv_wide + ssm_wide]
    values_raw = projected[:, cuts[1]:cuts[2]]
    attn_gate = projected[:, cuts[2]:cuts[3]]
    state_input = projected[:, cuts[3]:cuts[4]]
    state_gate = projected[:, cuts[4]:]

    half = HEAD_DIM // 2
    inv_freq = jnp.power(theta_base, -jnp.arange(half, dtype=jnp.float32) / half)
    angles = (offset + jnp.arange(extent, dtype=jnp.int32)).astype(jnp.float32)[:, None] * inv_freq
    repeats = cuts[1] // half
    cosine = jnp.tile(jnp.cos(angles), (1, repeats))
    sine = jnp.tile(jnp.sin(angles), (1, repeats))
    raw = projected[:, :cuts[1]]
    swapped = dot(raw, jnp.asarray(turn_matrix(cuts[1]), jnp.bfloat16))
    rotated = (raw.astype(jnp.float32) * cosine + swapped * sine).astype(jnp.bfloat16)
    queries = rotated[:, :q_wide]
    kv = jnp.concatenate([rotated[:, q_wide:], values_raw], axis=1)
    hop_count = (WINDOW + extent - 2) // extent
    near = jnp.concatenate([shifted(kv, "sp", d) for d in range(hop_count, 0, -1)] + [kv], axis=0)

    inputs_float = state_input.astype(jnp.float32)
    both = dot_exact(inputs_float, drive_in)
    pushes = times(inverse, (both[:, :states], both[:, states:]))
    lower = jnp.tril(jnp.ones((extent, extent), jnp.float32))
    running = dot_exact(lower, jnp.concatenate(pushes, axis=1))
    running = (running[:, :states], running[:, states:])
    last = times(tuple(f[-1:] for f in forward), tuple(r[-1:] for r in running))
    ending = jnp.concatenate(last, axis=0)
    arrivals = [shifted(ending, "sp", d) for d in range(1, count)]

    attended = window_attention(queries, near[:, :kv_wide], near[:, kv_wide:], sink_logits, offset, hop_count)
    gated_attn = (jax.nn.sigmoid(attn_gate.astype(jnp.float32)) * attended).astype(jnp.bfloat16)

    carry = (jnp.zeros_like(rate), jnp.zeros_like(rate))
    for arrival in reversed(arrivals):
        carry = times(whole_block, carry)
        carry = (carry[0] + arrival[0:1], carry[1] + arrival[1:2])
    entering = times(abar, carry)
    full = times(forward, (running[0] + entering[0], running[1] + entering[1]))
    reading = dot_exact(jnp.concatenate(full, axis=1), read_out) + skip_scale * inputs_float
    gated_state = (
        jax.nn.gelu(reading, approximate=False) * jax.nn.sigmoid(state_gate.astype(jnp.float32))
    ).astype(jnp.bfloat16)
    gated = jnp.concatenate([gated_attn, gated_state], axis=1)

    parts = [dot(gated, piece).astype(jnp.bfloat16) for piece in out_pieces]
    upward = [parts[0]] + parts[:0:-1]
    ordered = lax.dynamic_slice_in_dim(jnp.stack(upward + upward), count - mine, count, 0)
    fs_count, fs_mine = lax.axis_size("fs"), lax.axis_index("fs")
    blocks = jnp.transpose(ordered, (1, 0, 2)).reshape(extent, fs_count, width // fs_count)
    blocks = jnp.transpose(blocks, (1, 0, 2))
    pick = lambda d: lax.dynamic_index_in_dim(blocks, lax.rem(fs_mine + d, fs_count), 0, keepdims=False)
    received = [turned(pick(d), "fs", d) for d in range(1, fs_count)]
    mixed = pick(0).astype(jnp.float32)
    for piece in received:
        mixed = mixed + piece.astype(jnp.float32)
    sums = jnp.stack([jnp.sum(mixed, axis=-1), jnp.sum(mixed * mixed, axis=-1)])
    first_sum, second_sum = jnp.sum(lax.all_gather(sums, "fs"), axis=0)
    center = first_sum / width
    spread = second_sum / width - center * center
    result = (mixed - center[:, None]) * lax.rsqrt(spread[:, None] + epsilon) * out_gain
    return result.astype(jnp.bfloat16)[None]


def solution(mesh):
    placed = (
        P("tp", "sp", None),
        P(),
        P("sp", "fs"),
        P("sp", "fs"),
        P("sp", "fs"),
        P("sp", "fs"),
        P("sp", "fs"),
        P("sp", "fs"),
        P("fs"),
        P("fs", None),
        P("fs", None),
        P("fs"),
        P("fs", None, None),
        P("fs", None, None),
        P("fs", None, None),
        P("fs", None, None),
        P("fs"),
        P("fs", "sp"),
        P("fs", "sp"),
        P("fs"),
    )
    return jax.shard_map(
        on_device, mesh=mesh, in_specs=placed, out_specs=P("tp", "sp", "fs"), check_vma=False
    )
```

```python
import numpy as np
import jax
import jax.numpy as jnp
from jax import lax
from jax.sharding import PartitionSpec as P

HEAD_DIM = 64
WINDOW = 128
GROUP = 16

epsilon = 1e-05
theta_base = 10000.0


def shifted(value, axis, steps):
    count = lax.axis_size(axis)
    return lax.ppermute(value, axis, [(i, i + steps) for i in range(count - steps)])


def turned(value, axis, steps):
    count = lax.axis_size(axis)
    return lax.ppermute(value, axis, [(i, (i + steps) % count) for i in range(count)])


def swap(value, pairs):
    return lax.ppermute(value, "tp", [(i, i ^ 1) for i in range(2 * pairs)])


def dot(a, b):
    return jnp.dot(a, b, preferred_element_type=jnp.float32)


def dot_exact(a, b):
    return jnp.dot(a, b, preferred_element_type=jnp.float32, precision=lax.Precision.HIGHEST)


def times(a, b):
    return a[0] * b[0] - a[1] * b[1], a[0] * b[1] + a[1] * b[0]


def layer_norm(values, gain):
    center = jnp.mean(values, axis=-1, keepdims=True)
    spread = jnp.mean(jnp.square(values - center), axis=-1, keepdims=True)
    return (values - center) * lax.rsqrt(spread + epsilon) * gain


def turn_matrix(width):
    half = HEAD_DIM // 2
    matrix = np.zeros((width, width), np.float32)
    for column in range(width):
        if column % HEAD_DIM < half:
            matrix[column + half, column] = -1.0
        else:
            matrix[column - half, column] = 1.0
    return matrix


def powers(rate, angle, exponents):
    size = jnp.exp(exponents * rate)
    return size * jnp.cos(exponents * angle), size * jnp.sin(exponents * angle)


def spread_powers(rate, angle, count, sign):
    fine = 16 if count % 16 == 0 else count
    low = powers(rate, angle, sign * jnp.arange(fine, dtype=jnp.float32)[:, None])
    high = powers(rate, angle, sign * fine * jnp.arange(count // fine, dtype=jnp.float32)[:, None])
    product = times(tuple(h[:, None, :] for h in high), tuple(l[None] for l in low))
    return tuple(p.reshape(count, -1) for p in product)


def block_diagonal(blocks):
    groups, rows, columns = blocks.shape
    eye = jnp.eye(groups, dtype=blocks.dtype)
    return (blocks[:, :, None, :] * eye[:, None, :, None]).reshape(groups * rows, groups * columns)


def window_attention(queries, near_keys, near_values, sink_logits, offset, hop_count):
    extent = queries.shape[0]
    kv_local = near_keys.shape[1] // HEAD_DIM
    per_group = queries.shape[1] // HEAD_DIM // kv_local
    query_pos = offset + jnp.arange(extent, dtype=jnp.int32)
    key_pos = offset - hop_count * extent + jnp.arange((hop_count + 1) * extent, dtype=jnp.int32)
    differ = query_pos[:, None] - key_pos[None, :]
    allowed = (differ >= 0) & (differ < WINDOW) & (key_pos >= 0)[None, :]
    results = []
    for head in range(kv_local):
        keys = near_keys[:, head * HEAD_DIM:(head + 1) * HEAD_DIM]
        values = near_values[:, head * HEAD_DIM:(head + 1) * HEAD_DIM]
        start = head * per_group
        grouped = jnp.concatenate(
            [queries[:, (start + r) * HEAD_DIM:(start + r + 1) * HEAD_DIM] for r in range(per_group)], axis=0
        )
        scores = lax.dot_general(
            grouped, keys, (((1,), (1,)), ((), ())), preferred_element_type=jnp.float32
        ) * HEAD_DIM ** (-0.5)
        scores = scores.reshape(per_group, extent, -1)
        scores = jnp.where(allowed[None], scores, -jnp.inf)
        sink = sink_logits[start:start + per_group][:, None, None]
        largest = jnp.maximum(jnp.max(scores, axis=-1, keepdims=True), sink)
        weights = jnp.exp(scores - largest)
        weights = weights / (jnp.sum(weights, axis=-1, keepdims=True) + jnp.exp(sink - largest))
        weights = weights.astype(jnp.bfloat16).reshape(per_group * extent, -1)
        attended = dot(weights, values)
        results += [attended[r * extent:(r + 1) * extent] for r in range(per_group)]
    return jnp.concatenate(results, axis=1)


def on_device(
    tokens,
    in_gain,
    query_weight,
    key_weight,
    value_weight,
    attn_gate_weight,
    state_in_weight,
    state_gate_weight,
    sink_logits,
    decay_rate,
    rotation,
    step_size,
    input_real,
    input_imag,
    output_real,
    output_imag,
    skip_scale,
    focus_result_coefficients,
    state_out_weight,
    out_gain,
):
    extent, width = tokens.shape[1], tokens.shape[2]
    count = lax.axis_size("sp")
    mine = lax.axis_index("sp")
    offset = mine * extent
    total_length = extent * count
    own_in = jnp.concatenate(
        [query_weight, key_weight, value_weight, attn_gate_weight, state_in_weight, state_gate_weight], axis=1
    )
    own_out = jnp.concatenate([focus_result_coefficients, state_out_weight], axis=0)
    pairs = lax.axis_size("tp") // 2
    side = lax.rem(lax.axis_index("tp"), 2)
    half_in, half_out = own_in.shape[0] // 2, own_out.shape[0] // 2
    mine_in = lax.dynamic_slice_in_dim(own_in, side * half_in, half_in, 0)
    fetched = [turned(mine_in, "sp", d) for d in range(1, count)]
    swapped_in = [swap(piece, pairs) for piece in fetched]
    held_out, fetched[-1] = lax.optimization_barrier((own_out, fetched[-1]))
    mine_out = lax.dynamic_slice_in_dim(held_out, side * half_out, half_out, 0)
    fetched_out = jnp.stack([turned(mine_out, "sp", d) for d in range(1, count)])
    swapped_out = swap(fetched_out, pairs)

    step = jnp.repeat(step_size, decay_rate.shape[1])[None, :]
    states = decay_rate.shape[0] * decay_rate.shape[1]
    real_rate = -decay_rate.reshape(1, states) / total_length
    imag_rate = rotation.reshape(1, states)
    rate, angle = real_rate * step, imag_rate * step
    one = jnp.ones((1, 1), jnp.float32)
    abar = powers(rate, angle, one)
    denominator = real_rate * real_rate + imag_rate * imag_rate
    factor = (
        ((abar[0] - 1.0) * real_rate + abar[1] * imag_rate) / denominator,
        (abar[1] * real_rate - (abar[0] - 1.0) * imag_rate) / denominator,
    )
    forward = spread_powers(rate, angle, extent, 1.0)
    inverse = times(factor, spread_powers(rate, angle, extent, -1.0))
    whole_block = powers(rate, angle, extent * one)
    drive_in = jnp.concatenate(
        [block_diagonal(jnp.swapaxes(m, 1, 2)) for m in (input_real, input_imag)], axis=1
    )
    read_out = jnp.concatenate(
        [block_diagonal(jnp.swapaxes(m, 1, 2)) for m in (output_real, -output_imag)], axis=0
    )

    normed = layer_norm(tokens[0].astype(jnp.float32), in_gain).astype(jnp.bfloat16)
    depth = own_in.shape[0]
    columns = lambda start, size: lax.dynamic_slice_in_dim(normed, start, size, 1)
    totals = dot(columns(mine * depth, depth), own_in)
    for d in range(1, count):
        base = lax.rem(mine - d + count, count) * depth
        totals = totals + dot(columns(base + side * half_in, half_in), fetched[d - 1])
        totals = totals + dot(columns(base + (1 - side) * half_in, half_in), swapped_in[d - 1])
    projected = totals.astype(jnp.bfloat16)
    q_wide, kv_wide, ssm_wide = query_weight.shape[1], key_weight.shape[1], state_in_weight.shape[1]
    cuts = [q_wide, q_wide + kv_wide, q_wide + 2 * kv_wide, 2 * q_wide + 2 * kv_wide,
            2 * q_wide + 2 * kv_wide + ssm_wide]
    values_raw = projected[:, cuts[1]:cuts[2]]
    attn_gate = projected[:, cuts[2]:cuts[3]]
    state_input = projected[:, cuts[3]:cuts[4]]
    state_gate = projected[:, cuts[4]:]

    half = HEAD_DIM // 2
    inv_freq = jnp.power(theta_base, -jnp.arange(half, dtype=jnp.float32) / half)
    angles = (offset + jnp.arange(extent, dtype=jnp.int32)).astype(jnp.float32)[:, None] * inv_freq
    repeats = cuts[1] // half
    cosine = jnp.tile(jnp.cos(angles), (1, repeats))
    sine = jnp.tile(jnp.sin(angles), (1, repeats))
    raw = projected[:, :cuts[1]]
    swapped = dot(raw, jnp.asarray(turn_matrix(cuts[1]), jnp.bfloat16))
    rotated = (raw.astype(jnp.float32) * cosine + swapped * sine).astype(jnp.bfloat16)
    queries = rotated[:, :q_wide]
    kv = jnp.concatenate([rotated[:, q_wide:], values_raw], axis=1)
    hop_count = (WINDOW + extent - 2) // extent
    near = jnp.concatenate([shifted(kv, "sp", d) for d in range(hop_count, 0, -1)] + [kv], axis=0)

    inputs_float = state_input.astype(jnp.float32)
    both = dot_exact(inputs_float, drive_in)
    pushes = times(inverse, (both[:, :states], both[:, states:]))
    lower = jnp.tril(jnp.ones((extent, extent), jnp.float32))
    running = dot_exact(lower, jnp.concatenate(pushes, axis=1))
    running = (running[:, :states], running[:, states:])
    last = times(tuple(f[-1:] for f in forward), tuple(r[-1:] for r in running))
    ending = jnp.concatenate(last, axis=0)
    arrivals = [shifted(ending, "sp", d) for d in range(1, count)]

    attended = window_attention(queries, near[:, :kv_wide], near[:, kv_wide:], sink_logits, offset, hop_count)
    gated_attn = (jax.nn.sigmoid(attn_gate.astype(jnp.float32)) * attended).astype(jnp.bfloat16)

    carry = (jnp.zeros_like(rate), jnp.zeros_like(rate))
    for arrival in reversed(arrivals):
        carry = times(whole_block, carry)
        carry = (carry[0] + arrival[0:1], carry[1] + arrival[1:2])
    entering = times(abar, carry)
    full = times(forward, (running[0] + entering[0], running[1] + entering[1]))
    reading = dot_exact(jnp.concatenate(full, axis=1), read_out) + skip_scale * inputs_float
    gated_state = (
        jax.nn.gelu(reading, approximate=False) * jax.nn.sigmoid(state_gate.astype(jnp.float32))
    ).astype(jnp.bfloat16)
    gated = jnp.concatenate([gated_attn, gated_state], axis=1)

    gated_mine = lax.dynamic_slice_in_dim(gated, side * half_out, half_out, 1)
    gated_other = lax.dynamic_slice_in_dim(gated, (1 - side) * half_out, half_out, 1)
    parts = [dot(gated, own_out).astype(jnp.bfloat16)] + [
        (dot(gated_mine, fetched_out[d]) + dot(gated_other, swapped_out[d])).astype(jnp.bfloat16)
        for d in range(count - 1)
    ]
    upward = [parts[0]] + parts[:0:-1]
    ordered = lax.dynamic_slice_in_dim(jnp.stack(upward + upward), count - mine, count, 0)
    fs_count, fs_mine = lax.axis_size("fs"), lax.axis_index("fs")
    blocks = jnp.transpose(ordered, (1, 0, 2)).reshape(extent, fs_count, width // fs_count)
    blocks = jnp.transpose(blocks, (1, 0, 2))
    pick = lambda d: lax.dynamic_index_in_dim(blocks, lax.rem(fs_mine + d, fs_count), 0, keepdims=False)
    received = [turned(pick(d), "fs", d) for d in range(1, fs_count)]
    mixed = pick(0).astype(jnp.float32)
    for piece in received:
        mixed = mixed + piece.astype(jnp.float32)
    sums = jnp.stack([jnp.sum(mixed, axis=-1), jnp.sum(mixed * mixed, axis=-1)])
    first_sum, second_sum = jnp.sum(lax.all_gather(sums, "fs"), axis=0)
    center = first_sum / width
    spread = second_sum / width - center * center
    result = (mixed - center[:, None]) * lax.rsqrt(spread[:, None] + epsilon) * out_gain
    return result.astype(jnp.bfloat16)[None]


def solution(mesh):
    placed = (
        P("tp", "sp", None),
        P(),
        P("sp", "fs"),
        P("sp", "fs"),
        P("sp", "fs"),
        P("sp", "fs"),
        P("sp", "fs"),
        P("sp", "fs"),
        P("fs"),
        P("fs", None),
        P("fs", None),
        P("fs"),
        P("fs", None, None),
        P("fs", None, None),
        P("fs", None, None),
        P("fs", None, None),
        P("fs"),
        P("fs", "sp"),
        P("fs", "sp"),
        P("fs"),
    )
    return jax.shard_map(
        on_device, mesh=mesh, in_specs=placed, out_specs=P("tp", "sp", "fs"), check_vma=False
    )
```
